512 devices in a mesh: fs: 128 (over z, y, core), tp: 4 (over x).
Axes of the slice: x: 4, y: 8, z: 8, core: 2. Of those that a mesh axis runs over, the one named last changes fastest.
Arguments:
- rnn_out: bfloat16 [98304, 1536], P('fs', 'tp'), may hold values from -6 to 6
- out_grad: bfloat16 [98304, 2048], P('fs', 'tp'), may hold values from -0.078125 to 0.078125
- weight: float32 [2048, 1536], P('fs', 'tp'), may hold values from -0.15625 to 0.15625
- left_root: bfloat16 [4, 2048, 2048], P('tp', 'fs'), as said below
- right_root: bfloat16 [4, 384, 384], P('tp'), as said below
- left_stat: float32 [4, 2048, 2048], P('tp', 'fs'), may hold values from -4 to 4
- right_stat: float32 [4, 384, 384], P('tp', 'fs'), may hold values from -4 to 4
Outputs:
- new_weight: float32 [2048, 1536], P('fs', 'tp')
- step: float32 [2048, 1536], P('fs', 'tp')
- left_new: float32 [4, 2048, 2048], P('tp', 'fs')
- right_new: float32 [4, 384, 384], P('tp', 'fs')
- weight_copy: bfloat16 [2048, 1536], P(None, 'tp')
The draws below stay inside these ranges and needn't reach their ends.
Inputs may be any that keep to these rules, and one draw needn't show every extreme that they name: `left_root`: each block is symmetric. `right_root`: each block is symmetric.
All inputs are finite; a program needn't handle non-finite values.
Results may differ from the reference program's by a relative error of at most 0.0049.
Values may be sent and summed in bfloat16 or wider, within the bound.
A program may use at most 64 MiB of HBM per device.

```python
import jax
import jax.numpy as jnp

D = 2048
R = 1536
TOKENS = 98304
NB = 4
RB = 384


def symmetric_root(key, width):
    noise = jax.random.normal(key, (NB, width, width), jnp.float32)
    mixed = (noise + jnp.swapaxes(noise, 1, 2)) * (0.5 / (2.0 * width) ** 0.5)
    matrix = jnp.eye(width, dtype=jnp.float32)[None] + mixed
    return matrix


def draw_left_root(key, part):
    return symmetric_root(jax.random.fold_in(key, 11), D).astype(jnp.bfloat16)


def draw_right_root(key, part):
    return symmetric_root(jax.random.fold_in(key, 23), RB).astype(jnp.bfloat16)


def spiked(values, own_key, source, target, blocks, factor):
    def block_of(position):
        return (jnp.arange(values.shape[position]) // (values.shape[position] // blocks)).reshape((-1,) + (1,) * (values.ndim - 1 - position))

    first = jax.random.permutation(own_key, blocks)[block_of(target)]
    second = (block_of(target) + blocks // 2) % blocks
    return jnp.where((block_of(source) == first) | (block_of(source) == second), factor * values, values)


def block_levels(rng, shape, cuts, smallest, top_value):
    def one(position, shards_of):
        heights = jax.random.uniform(jax.random.fold_in(jax.random.fold_in(rng, 6), position), (shards_of,), jnp.float32, smallest / len(cuts), top_value / len(cuts))
        return jnp.repeat(jnp.exp(heights), shape[position] // shards_of).reshape((-1,) + (1,) * (len(shape) - position - 1))

    factor_of = one(*cuts[0])
    for cut in cuts[1:]:
        factor_of = factor_of * one(*cut)
    return factor_of


def normal_values(own_key, extent, scale, most, split=(), kind=jnp.bfloat16):
    result = scale * jax.random.normal(own_key, extent, jnp.float32)
    if split:
        result = result * block_levels(own_key, extent, split, -0.22, 0.18)
    return jnp.clip(result, -most, most).astype(kind)


def heavy_noise(rng, extent, scale, reach, pieces, heavy, kind=jnp.bfloat16):
    entries = scale * jax.random.normal(rng, extent, jnp.float32)
    if pieces:
        entries = entries * block_levels(rng, extent, pieces, -0.22, 0.18)
    return jnp.clip(spiked(entries, jax.random.fold_in(rng, 3), *heavy), -reach, reach).astype(kind)


def setup_inputs(seed: int = 0) -> dict:
    streams_of = jax.random.split(jax.random.key(seed), 8)
    rnn_out = normal_values(streams_of[0], (TOKENS, R), 1.0, 6.0, ((0, 128), (1, 4)))
    out_grad = heavy_noise(streams_of[1], (TOKENS, D), (1.0 / TOKENS ** 0.5), 0.078125, ((0, 128), (1, 4)), (0, 1, 128, 5.5))
    weight = normal_values(streams_of[2], (D, R), R ** -0.5, 0.15625, ((0, 128), (1, 4)), jnp.float32)
    left_root = draw_left_root(jax.random.fold_in(streams_of[7], 71), 0)
    right_root = draw_right_root(jax.random.fold_in(streams_of[7], 71), 0)
    left_stat = normal_values(streams_of[5], (NB, D, D), 0.5, 4.0, ((0, 4), (1, 128)), jnp.float32)
    right_stat = normal_values(streams_of[6], (NB, RB, RB), 0.5, 4.0, ((0, 4), (1, 128)), jnp.float32)
    return dict(rnn_out=rnn_out, out_grad=out_grad, weight=weight, left_root=left_root, right_root=right_root, left_stat=left_stat, right_stat=right_stat)


decay_rate = 0.8
step_size = 0.005

def reference(rnn_out, out_grad, weight, left_root, right_root, left_stat, right_stat):
    grad = jnp.dot(out_grad.T, rnn_out, preferred_element_type=jnp.float32)
    grad_low = grad.astype(jnp.bfloat16)
    grad_square = jnp.sum(grad * grad)
    lefts = []
    rights = []
    updates = []
    for index in range(NB):
        column = grad_low[:, index * RB:(index + 1) * RB]
        outer = jnp.dot(column, column.T, preferred_element_type=jnp.float32) / RB
        inner = jnp.dot(column.T, column, preferred_element_type=jnp.float32) / D
        lefts.append(decay_rate * left_stat[index] + (1.0 - decay_rate) * outer)
        rights.append(decay_rate * right_stat[index] + (1.0 - decay_rate) * inner)
        applied = jnp.dot(left_root[index], column, preferred_element_type=jnp.float32).astype(jnp.bfloat16)
        updates.append(jnp.dot(applied, right_root[index], preferred_element_type=jnp.float32))
    update = jnp.concatenate(updates, axis=1)
    scale = jnp.sqrt(grad_square + 1.0) / jnp.sqrt(jnp.sum(update * update) + 1.0)
    step = scale * update
    new_weight = weight - step_size * step
    return (new_weight, step, jnp.stack(lefts), jnp.stack(rights), new_weight.astype(jnp.bfloat16))
```

```python
import functools

import jax
import jax.numpy as jnp
from jax import lax
from jax.experimental import pallas as pl
from jax.experimental.pallas import tpu as pltpu
from jax.sharding import Mesh
from jax.sharding import PartitionSpec as P

FS = ("fs_0", "fs_1", "fs_2")
MESH = pl.DeviceIdType.MESH
N = 8
F32 = jnp.float32
BF16 = jnp.bfloat16

decay_rate = 0.8
step_size = 0.005


def kernel(
    rnn_hbm, cot_hbm, w_hbm, lroot_hbm, rroot_hbm, lstat_hbm, rstat_hbm,
    nw_hbm, step_hbm, left_hbm, right_hbm, wc_hbm,
    rnn_own, rnn_in, cot_own, cot_in, w_v, lroot, rroot, lstat, rstat,
    part, part_in, rs1_out, rs1_in, rs2_out, rs2_in, G, A, W, upd, sc_own, sc_in,
    nw_v, step_v, left_v, right_v, wc_v,
    load_sem, store_sem,
    x_s, x_r, d2d_s, d2d_r, rs1_s, rs1_r, rs2_s, rs2_r,
    p1_s, p1_r, p2_s, p2_r, fw_s, fw_r, sc_s, sc_r,
):
    z, y, c, x = (lax.axis_index(a) for a in ("fs_0", "fs_1", "fs_2", "tp"))
    rem = lax.rem
    o = y + c * (z - y)
    i = z + c * (y - z)
    x_rnn = x + 1 - 2 * rem(x, 2)
    x_cot = 3 - x
    q_me, h_me = i // 2, rem(i, 2)
    odd_me = rem(q_me, 2)
    high = rem(x // 2 + q_me // 2, 2)
    low = rem(rem(x, 2) + rem((q_me + 1) // 2, 2), 2)
    blk_me = 2 * high + low

    def outer(k):
        return (rem(z + c * k, N), rem(y + (1 - c) * k, N), c, x)

    def inner(k):
        return (rem(z + (1 - c) * k, N), rem(y + c * k, N), c, x)

    def inner_at(j, xx):
        return (z + (1 - c) * (j - z), y + c * (j - y), c, xx)

    partner = (z, y, 1 - c, x)

    def remote(src, dst, s, r, to):
        return pltpu.make_async_remote_copy(
            src_ref=src, dst_ref=dst, send_sem=s, recv_sem=r, device_id=to, device_id_type=MESH
        )

    def settle(ref, sem):
        pltpu.make_async_copy(ref, ref, sem).wait()

    loads = [
        pltpu.make_async_copy(src, dst, load_sem.at[n])
        for n, (src, dst) in enumerate(
            [(cot_hbm, cot_own), (rnn_hbm, rnn_own), (w_hbm, w_v), (rroot_hbm, rroot), (lroot_hbm, lroot),
             (lstat_hbm, lstat), (rstat_hbm, rstat)]
        )
    ]
    for load in loads:
        load.start()

    barrier = pltpu.get_barrier_semaphore()

    def greet(k, _):
        pl.semaphore_signal(barrier, inc=1, device_id=outer(k), device_id_type=MESH)
        pl.semaphore_signal(barrier, inc=1, device_id=inner(k), device_id_type=MESH)
        zi, yi, _, _ = inner(k)
        pl.semaphore_signal(barrier, inc=1, device_id=(zi, yi, c, x_rnn), device_id_type=MESH)
        return 0

    lax.fori_loop(1, N, greet, 0)
    for k in range(1, 4):
        pl.semaphore_signal(barrier, inc=1, device_id=(z, y, c, rem(x + k, 4)), device_id_type=MESH)
    pl.semaphore_signal(barrier, inc=1, device_id=partner, device_id_type=MESH)
    pl.semaphore_wait(barrier, 3 * (N - 1) + 4)

    x_copies = []
    loads[0].wait()
    for h in range(2):
        cols = pl.ds(256 * h, 256)
        x_copies.append(remote(cot_own.at[:, cols], cot_in.at[h], x_s.at[h], x_r.at[h], (z, y, c, x_cot)))
    loads[1].wait()
    x_copies.append(remote(rnn_own, rnn_in, x_s.at[2], x_r.at[2], (z, y, c, x_rnn)))
    for n in (0, 2, 1):
        x_copies[n].start()

    def gather_1(t, mine):
        def send(k, _):
            remote(mine, mine, p1_s.at[t], p1_r.at[t], inner(k)).start()
            return 0

        lax.fori_loop(1, N, send, 0)

    def gather_2(t, block, both):
        settle(both.at[pl.ds(0, N - 1)], p1_r.at[t])
        settle(both.at[pl.ds(0, N - 1)], p1_s.at[t])

        def send(k, _):
            remote(block, block, p2_s.at[t, k], p2_r.at[t, k], outer(rem(k + 3, N - 1) + 1)).start()
            return 0

        lax.fori_loop(0, N - 1, send, 0)
        remote(block, block, fw_s.at[t], fw_r.at[t], partner).start()

    def gather_3(t, at, sized):
        def forward(k, _):
            off = rem(k + 3, N - 1) + 1
            src = rem(o - off + N, N)
            settle(at(src), p2_r.at[t, k])
            remote(at(src), at(src), fw_s.at[t], fw_r.at[t], partner).start()
            return 0

        lax.fori_loop(0, N - 1, forward, 0)

    def gather_4(t, at, sized):
        settle(sized, fw_r.at[t])
        settle(sized, fw_s.at[t])

        def sent(k, _):
            settle(at(o), p2_s.at[t, k])
            return 0

        lax.fori_loop(0, N - 1, sent, 0)

    loads[2].wait()
    W[c, o, i] = w_v[...].astype(BF16)
    gather_1(0, W.at[c, o, i])

    def product(cot, rnn):
        return lax.dot_general(cot, rnn, (((0,), (0,)), ((), ())), preferred_element_type=F32)

    def d2d(j):
        return remote(part.at[j, 1 - c], part_in.at[j], d2d_s.at[j], d2d_r.at[j], partner)

    def compute(j):
        q, h = j // 2, j % 2
        cot = cot_own[:, 256 * h:256 * h + 256] if q < 2 else cot_in[h]
        rnn = rnn_own[...] if q % 2 == 0 else rnn_in[...]
        part[j] = product(cot, rnn).reshape(2, N, 16, 384)
        d2d(j).start()

    def scatter_1(j):
        d2d(j).wait_recv()
        both = part[j, c] + part_in[j]
        part_in[j] = both
        rs1_out[j] = both.astype(BF16)

        def send(k, _):
            remote(rs1_out.at[j, rem(o + k, N)], rs1_in.at[j, k - 1], rs1_s.at[j], rs1_r.at[j], outer(k)).start()
            return 0

        lax.fori_loop(1, N, send, 0)

    def scatter_2(j):
        settle(rs1_in.at[j], rs1_r.at[j])
        total = part_in[j, o]
        for k in range(N - 1):
            total = total + rs1_in[j, k].astype(F32)
        rs2_out[j] = total
        odd = (j // 2) % 2 == 1
        if odd:
            remote(rs2_out.at[j], rs2_in.at[i], rs2_s.at[j], rs2_r.at[i], inner_at(j, x_rnn)).start()
        else:
            @pl.when(i != j)
            def _():
                remote(rs2_out.at[j], rs2_in.at[i], rs2_s.at[j], rs2_r.at[i], inner_at(j, x)).start()

            @pl.when(i == j)
            def _():
                rs2_in[i] = total

    compute(0)
    compute(1)
    scatter_1(0)
    scatter_1(1)
    gather_2(0, W.at[c, o], W.at[c, o])
    x_copies[0].wait_recv()
    compute(4)
    scatter_2(0)
    scatter_2(1)
    scatter_1(4)
    gather_3(0, lambda s: W.at[c, s], None)
    x_copies[2].wait_recv()
    compute(2)
    compute(3)
    compute(6)
    scatter_1(2)
    scatter_1(3)
    scatter_1(6)
    scatter_2(4)
    x_copies[1].wait_recv()
    compute(5)
    compute(7)
    scatter_2(2)
    scatter_2(3)
    scatter_2(6)
    scatter_1(5)
    scatter_1(7)
    scatter_2(5)
    scatter_2(7)

    def arrived(s, _):
        @pl.when((odd_me == 1) | (s != i))
        def _():
            settle(rs2_in.at[s], rs2_r.at[s])

        return 0

    lax.fori_loop(0, N, arrived, 0)
    piece = rs2_in[0]
    for s in range(1, N):
        piece = piece + rs2_in[s]
    G[blk_me, h_me, c, o] = piece.astype(BF16)
    gather_1(1, G.at[blk_me, h_me, c, o])
    loads[3].wait()
    loads[4].wait()
    loads[5].wait()
    loads[6].wait()
    gather_2(1, G.at[:, :, c, o], W.at[c, o])
    gather_3(1, lambda s: G.at[:, :, c, s], None)
    gather_4(1, lambda s: G.at[:, :, c, s], G.at[:, :, 1 - c])

    grad = G[...].reshape(2048, 384)
    rows = jnp.dot(lroot[...], grad, preferred_element_type=F32)
    A[c, o, i] = rows.astype(BF16)
    gather_1(2, A.at[c, o, i])

    gsq = jnp.zeros((128, 384), F32)
    for b in range(4):
        for h in range(2):
            for s in range(2):
                block = G[b, h, s].reshape(128, 384).astype(F32)
                gsq = gsq + block * block
    gather_2(2, A.at[c, o], A.at[c, o])

    index = (z * N + y) * 2 + c
    own = G[z // 2, rem(z, 2), y // 4, rem(y, 4) * 2 + c]
    outer_sum = lax.dot_general(own, grad, (((1,), (1,)), ((), ())), preferred_element_type=F32)
    left_v[...] = decay_rate * lstat[...] + (1.0 - decay_rate) * (outer_sum / 384)
    pick_row = lax.broadcasted_iota(jnp.int32, (16, 384), 0)
    pick_col = lax.broadcasted_iota(jnp.int32, (16, 384), 1)
    pick = jnp.where((pick_col == 3 * index + pick_row) & (pick_row < 3), 1.0, 0.0).astype(BF16)
    columns = lax.dot_general(pick, grad, (((1,), (1,)), ((), ())), preferred_element_type=F32).astype(BF16)
    right_sum = jnp.dot(columns, grad, preferred_element_type=F32)
    right_v[...] = decay_rate * rstat[...] + (1.0 - decay_rate) * (right_sum[0:3] / 2048)
    stores = [
        pltpu.make_async_copy(left_v, left_hbm, store_sem.at[0]),
        pltpu.make_async_copy(right_v, right_hbm, store_sem.at[1]),
    ]
    for store in stores:
        store.start()

    gather_3(2, lambda s: A.at[c, s], None)
    gather_4(2, lambda s: A.at[c, s], A.at[1 - c])

    usq = jnp.zeros((128, 384), F32)
    for cc in range(2):
        for oo in range(N):
            value = jnp.dot(A[cc, oo].reshape(128, 384), rroot[...], preferred_element_type=F32)
            upd[cc, oo] = value.reshape(N, 16, 384)
            usq = usq + value * value
    line = lax.broadcasted_iota(jnp.int32, (8, 128), 0)
    sc_own[...] = jnp.where(line == 0, jnp.sum(gsq), jnp.sum(usq))
    for k in range(1, 4):
        remote(sc_own, sc_in.at[k - 1], sc_s.at[k - 1], sc_r.at[k - 1], (z, y, c, rem(x + k, 4))).start()

    gather_4(0, lambda s: W.at[c, s], W.at[1 - c])

    for k in range(3):
        settle(sc_own, sc_r.at[k])
    sums = sc_own[...] + sc_in[0] + sc_in[1] + sc_in[2]
    scale = jnp.sqrt(sums[0:1, 0:1] + 1.0) / jnp.sqrt(sums[1:2, 0:1] + 1.0)
    step = scale * upd[c, o, i]
    step_v[...] = step
    nw_v[...] = w_v[...] - step_size * step
    stores.append(pltpu.make_async_copy(step_v, step_hbm, store_sem.at[2]))
    stores.append(pltpu.make_async_copy(nw_v, nw_hbm, store_sem.at[3]))
    stores[2].start()
    stores[3].start()
    for oo in range(N):
        for ii in range(N):
            first = W[0, oo, ii].astype(F32) - step_size * (scale * upd[0, oo, ii])
            wc_v[ii, oo, 0] = first.astype(BF16)
            second = W[1, oo, ii].astype(F32) - step_size * (scale * upd[1, oo, ii])
            wc_v[oo, ii, 1] = second.astype(BF16)
    stores.append(pltpu.make_async_copy(wc_v, wc_hbm, store_sem.at[4]))
    stores[4].start()

    for n in range(3):
        x_copies[n].wait_send()
        settle(sc_own, sc_s.at[n])
    for j in range(N):
        d2d(j).wait_send()
        settle(rs1_in.at[j], rs1_s.at[j])
        if (j // 2) % 2 == 1:
            settle(rs2_out.at[j], rs2_s.at[j])
        else:
            @pl.when(i != j)
            def _():
                settle(rs2_out.at[j], rs2_s.at[j])

    for store in stores:
        store.wait()


def body(rnn_out, out_grad, weight, left_root, right_root, left_stat, right_stat):
    tokens = rnn_out.shape[0]
    hbm = pl.BlockSpec(memory_space=pl.ANY)
    v = pltpu.VMEM
    dma = pltpu.SemaphoreType.DMA
    outs = pl.pallas_call(
        kernel,
        name="step",
        out_shape=(
            jax.ShapeDtypeStruct((16, 384), F32),
            jax.ShapeDtypeStruct((16, 384), F32),
            jax.ShapeDtypeStruct((16, 2048), F32),
            jax.ShapeDtypeStruct((3, 384), F32),
            jax.ShapeDtypeStruct((N, N, 2, 16, 384), BF16),
        ),
        in_specs=[hbm] * 7,
        out_specs=(hbm,) * 5,
        scratch_shapes=[
            v((tokens, 384), BF16), v((tokens, 384), BF16), v((tokens, 512), BF16), v((2, tokens, 256), BF16),
            v((16, 384), F32), v((16, 2048), BF16), v((384, 384), BF16), v((16, 2048), F32), v((3, 384), F32),
            v((N, 2, N, 16, 384), F32), v((N, N, 16, 384), F32),
            v((N, N, 16, 384), BF16), v((N, N - 1, 16, 384), BF16),
            v((N, 16, 384), F32), v((N, 16, 384), F32),
            v((4, 2, 2, N, 16, 384), BF16), v((2, N, N, 16, 384), BF16), v((2, N, N, 16, 384), BF16),
            v((2, N, N, 16, 384), F32), v((8, 128), F32), v((3, 8, 128), F32),
            v((16, 384), F32), v((16, 384), F32), v((16, 2048), F32), v((3, 384), F32), v((N, N, 2, 16, 384), BF16),
            dma((7,)), dma((5,)),
            dma((3,)), dma((3,)), dma((N,)), dma((N,)), dma((N,)), dma((N,)), dma((N,)), dma((N,)),
            dma((3,)), dma((3,)), dma((3, N - 1)), dma((3, N - 1)), dma((3,)), dma((3,)), dma((3,)), dma((3,)),
        ],
        compiler_params=pltpu.CompilerParams(collective_id=0, has_side_effects=True),
    )(rnn_out, out_grad, weight, left_root[0], right_root[0], left_stat[0], right_stat[0])
    new_weight, step, left_new, right_new, copy = outs
    return new_weight, step, left_new[None], right_new[None], copy.reshape(2048, 384)


def solution(mesh):
    torus = Mesh(mesh.devices.reshape(N, N, 2, mesh.shape["tp"]), ("fs_0", "fs_1", "fs_2", "tp"))
    return jax.shard_map(
        body,
        mesh=torus,
        in_specs=(
            P(FS, "tp"),
            P(FS, "tp"),
            P(FS, "tp"),
            P("tp", FS, None),
            P("tp", None, None),
            P("tp", FS, None),
            P("tp", FS, None),
        ),
        out_specs=(P(FS, "tp"), P(FS, "tp"), P("tp", FS, None), P("tp", FS, None), P(None, "tp")),
        check_vma=False,
    )
```

```python
import functools

import jax
import jax.numpy as jnp
from jax import lax
from jax.experimental import pallas as pl
from jax.experimental.pallas import tpu as pltpu
from jax.sharding import Mesh
from jax.sharding import PartitionSpec as P

FS = ("fs_0", "fs_1", "fs_2")
MESH = pl.DeviceIdType.MESH
N = 8
F32 = jnp.float32
BF16 = jnp.bfloat16

decay_rate = 0.8
step_size = 0.005


def kernel(
    rnn_hbm, cot_hbm, w_hbm, lroot_hbm, rroot_hbm, lstat_hbm, rstat_hbm,
    nw_v, step_v, left_v, right_v, wc_v,
    rnn_own, rnn_in, cot_own, cot_in, w_v, lroot, rroot, lstat, rstat,
    part, part_in, rs1_out, rs1_in, ar_out, ar_in, G, A, W, upd, own_update, piece_v, t1, t2, t3, t3_in, t4,
    load_sem,
    x_s, x_r, d2d_s, d2d_r, rs1_s, rs1_r, ar_s, ar_r,
    g2_s, g2_r, g3_s, g3_r, a1_s, a1_r, a2_s, a2_r, a3_s, a3_r,
    w1_s, w1_r, w2_s, w2_r, w3_s, w3_r, t_s, t_r,
):
    z, y, c, x = (lax.axis_index(a) for a in ("fs_0", "fs_1", "fs_2", "tp"))
    rem = lax.rem
    o = y + c * (z - y)
    i = z + c * (y - z)
    x_rnn = x + 1 - 2 * rem(x, 2)
    x_cot = 3 - x
    blocks = (x, x_rnn, x_cot, rem(x + 2, 4))

    def outer(k):
        return (rem(z + c * k, N), rem(y + (1 - c) * k, N), c, x)

    def inner(k, xx=None):
        return (rem(z + (1 - c) * k, N), rem(y + c * k, N), c, x if xx is None else xx)

    def along_x(k):
        return (z, y, c, rem(x + k, 4))

    partner = (z, y, 1 - c, x)

    def remote(src, dst, s, r, to):
        return pltpu.make_async_remote_copy(
            src_ref=src, dst_ref=dst, send_sem=s, recv_sem=r, device_id=to, device_id_type=MESH
        )

    def settle(ref, sem):
        pltpu.make_async_copy(ref, ref, sem).wait()

    def to_all(ref, s, r, peers, count=N):
        def send(k, _):
            remote(ref, ref, s, r, peers(k)).start()
            return 0

        lax.fori_loop(1, count, send, 0)

    seven = rs1_in.at[0]

    loads = [
        pltpu.make_async_copy(src, dst, load_sem.at[n])
        for n, (src, dst) in enumerate(
            [(cot_hbm, cot_own), (rnn_hbm, rnn_own), (w_hbm, w_v), (rroot_hbm, rroot), (lroot_hbm, lroot),
             (lstat_hbm, lstat), (rstat_hbm, rstat)]
        )
    ]
    for load in loads:
        load.start()

    barrier = pltpu.get_barrier_semaphore()

    def greet(k, _):
        pl.semaphore_signal(barrier, inc=1, device_id=outer(k), device_id_type=MESH)
        pl.semaphore_signal(barrier, inc=1, device_id=inner(k), device_id_type=MESH)
        zi, yi, _, _ = inner(k)
        pl.semaphore_signal(barrier, inc=1, device_id=(zi, yi, c, x_rnn), device_id_type=MESH)
        return 0

    lax.fori_loop(1, N, greet, 0)
    for k in range(1, 4):
        pl.semaphore_signal(barrier, inc=1, device_id=along_x(k), device_id_type=MESH)
    pl.semaphore_signal(barrier, inc=1, device_id=partner, device_id_type=MESH)
    pl.semaphore_wait(barrier, 3 * (N - 1) + 4)

    x_copies = []
    loads[0].wait()
    for h in range(2):
        cols = pl.ds(256 * h, 256)
        x_copies.append(remote(cot_own.at[:, cols], cot_in.at[h], x_s.at[h], x_r.at[h], (z, y, c, x_cot)))
    loads[1].wait()
    x_copies.append(remote(rnn_own, rnn_in, x_s.at[2], x_r.at[2], (z, y, c, x_rnn)))
    for n in (0, 2, 1):
        x_copies[n].start()

    def weight_1():
        loads[2].wait()
        W[c, i, o] = w_v[...].astype(BF16)
        to_all(W.at[c, i, o], w1_s, w1_r, inner)

    def weight_2():
        settle(seven, w1_r)

        def send(k, _):
            row = W.at[c, :, o]
            remote(row, row, w2_s.at[k], w2_r.at[k], outer(rem(k + 3, N - 1) + 1)).start()
            return 0

        lax.fori_loop(0, N - 1, send, 0)

    def weight_3():
        def arrive(k, _):
            settle(W.at[c, :, o], w2_r.at[k])
            return 0

        lax.fori_loop(0, N - 1, arrive, 0)
        remote(W.at[c], W.at[c], w3_s, w3_r, partner).start()

    def product(cot, rnn):
        return lax.dot_general(cot, rnn, (((0,), (0,)), ((), ())), preferred_element_type=F32)

    def d2d(j):
        return remote(part.at[j, 1 - c], part_in.at[j], d2d_s.at[j], d2d_r.at[j], partner)

    def compute(j):
        q, h = j // 2, j % 2
        cot = cot_own[:, 256 * h:256 * h + 256] if q < 2 else cot_in[h]
        rnn = rnn_own[...] if q % 2 == 0 else rnn_in[...]
        part[j] = product(cot, rnn).reshape(2, N, 16, 384)
        d2d(j).start()

    def scatter_1(j):
        d2d(j).wait_recv()
        both = part[j, c] + part_in[j]
        part_in[j] = both
        rs1_out[j] = both.astype(BF16)

        def send(k, _):
            remote(rs1_out.at[j, rem(o + k, N)], rs1_in.at[j, k - 1], rs1_s.at[j], rs1_r.at[j], outer(k)).start()
            return 0

        lax.fori_loop(1, N, send, 0)

    def scatter_2(j):
        settle(seven, rs1_r.at[j])
        total = part_in[j, o]
        for k in range(N - 1):
            total = total + rs1_in[j, k].astype(F32)
        mine = total.astype(BF16)
        if (j // 2) % 2 == 1:
            ar_out[j] = mine

            def send(k, _):
                remote(ar_out.at[j], ar_in.at[j, i], ar_s.at[j], ar_r.at[j], inner(k, x_rnn)).start()
                return 0

            lax.fori_loop(0, N, send, 0)
        else:
            ar_in[j, i] = mine
            to_all(ar_in.at[j, i], ar_s.at[j], ar_r.at[j], inner)

    def g_piece(j):
        return G.at[blocks[j // 2], j % 2, c, o]

    def gather_2(j):
        settle(ar_in.at[j] if (j // 2) % 2 == 1 else seven, ar_r.at[j])
        piece = ar_in[j, 0].astype(F32)
        for s in range(1, N):
            piece = piece + ar_in[j, s].astype(F32)
        G[blocks[j // 2], j % 2, c, o] = piece.astype(BF16)

        @pl.when(i == j)
        def _():
            piece_v[...] = piece

        to_all(g_piece(j), g2_s.at[j], g2_r.at[j], outer)

    def gather_3(j):
        settle(seven, g2_r.at[j])
        both = G.at[blocks[j // 2], j % 2, c]
        remote(both, both, g3_s, g3_r, partner).start()

    weight_1()
    compute(0)
    compute(1)
    scatter_1(0)
    scatter_1(1)
    weight_2()
    x_copies[0].wait_recv()
    compute(4)
    scatter_2(0)
    scatter_2(1)
    scatter_1(4)
    x_copies[2].wait_recv()
    compute(2)
    compute(3)
    compute(6)
    scatter_1(2)
    scatter_1(3)
    scatter_1(6)
    gather_2(0)
    gather_2(1)
    scatter_2(4)
    x_copies[1].wait_recv()
    compute(5)
    compute(7)
    scatter_1(5)
    scatter_1(7)
    scatter_2(2)
    scatter_2(3)
    scatter_2(6)
    gather_2(4)
    scatter_2(5)
    scatter_2(7)
    gather_2(2)
    gather_2(3)
    gather_2(6)
    gather_3(0)
    gather_3(1)
    weight_3()
    gather_2(5)
    gather_2(7)
    gather_3(4)
    gather_3(2)
    gather_3(3)
    gather_3(6)
    gather_3(5)
    gather_3(7)
    for n in range(3, 7):
        loads[n].wait()
    settle(W.at[0], g3_r)

    grad = G[...].reshape(2048, 384)
    rows = jnp.dot(lroot[...], grad, preferred_element_type=F32).astype(BF16)
    A[c, i, o] = rows
    to_all(A.at[c, i, o], a1_s, a1_r.at[i], inner)

    update = jnp.dot(rows, rroot[...], preferred_element_type=F32)
    own_update[...] = update
    line = lax.broadcasted_iota(jnp.int32, (8, 128), 0)
    t1[o] = jnp.where(line == 0, jnp.sum(piece_v[...] * piece_v[...]), jnp.sum(update * update))
    to_all(t1.at[o], t_s.at[0], t_r.at[0], outer)
    to_all(A.at[c, i, o], a2_s.at[i], a2_r.at[i], outer)

    def relay(k, _):
        half = (k + 1) // 2
        j = rem(i + half + rem(k + 1, 2) * (N - 2 * half), N)
        settle(A.at[c, j, o], a1_r.at[j])
        to_all(A.at[c, j, o], a2_s.at[j], a2_r.at[j], outer)
        return 0

    lax.fori_loop(1, 5, relay, 0)

    def total_of(ref, count):
        total = ref[0]
        for s in range(1, count):
            total = total + ref[s]
        return total

    settle(t1.at[pl.ds(0, N - 1)], t_r.at[0])
    t2[i] = total_of(t1, N)
    to_all(t2.at[i], t_s.at[1], t_r.at[1], inner)
    lax.fori_loop(5, N, relay, 0)

    index = (z * N + y) * 2 + c
    own = G[z // 2, rem(z, 2), y // 4, rem(y, 4) * 2 + c]
    outer_sum = lax.dot_general(own, grad, (((1,), (1,)), ((), ())), preferred_element_type=F32)
    left_v[...] = decay_rate * lstat[...] + (1.0 - decay_rate) * (outer_sum / 384)
    pick_row = lax.broadcasted_iota(jnp.int32, (16, 384), 0)
    pick_col = lax.broadcasted_iota(jnp.int32, (16, 384), 1)
    pick = jnp.where((pick_col == 3 * index + pick_row) & (pick_row < 3), 1.0, 0.0).astype(BF16)
    columns = lax.dot_general(pick, grad, (((1,), (1,)), ((), ())), preferred_element_type=F32).astype(BF16)
    right_sum = jnp.dot(columns, grad, preferred_element_type=F32)
    for r in range(3):
        right_v[r] = decay_rate * rstat[r] + (1.0 - decay_rate) * (right_sum[r:r + 1] / 2048)

    settle(t2.at[pl.ds(0, N - 1)], t_r.at[1])
    t3[...] = total_of(t2, N)
    remote(t3, t3_in, t_s.at[2], t_r.at[2], partner).start()

    def pass_on(k):
        j = near(i, k)
        settle(seven, a2_r.at[j])
        remote(A.at[c, j], A.at[c, j], a3_s, a3_r.at[j], partner).start()
        multiply(c, j)

    def near(start, k):
        half = (k + 1) // 2
        return rem(start + half + ((k + 1) % 2) * (N - 2 * half), N)

    def multiply(core, j):
        upd[core, j] = jnp.dot(
            A[core, j].reshape(128, 384), rroot[...], preferred_element_type=F32
        ).reshape(N, 16, 384)

    def take(k):
        j = near(o, k)
        settle(A.at[c, j], a3_r.at[j])
        multiply(1 - c, j)

    pass_on(0)
    pass_on(1)
    pass_on(2)
    settle(t3, t_r.at[2])
    t4[x] = t3[...] + t3_in[...]
    to_all(t4.at[x], t_s.at[3], t_r.at[3], along_x, 4)
    pass_on(3)
    take(0)
    pass_on(4)
    take(1)
    take(2)
    pass_on(5)
    take(3)
    pass_on(6)
    take(4)
    pass_on(7)
    take(5)
    settle(W.at[1 - c], w3_r)
    settle(t4.at[pl.ds(0, 3)], t_r.at[3])
    sums = total_of(t4, 4)
    scale = jnp.sqrt(sums[0:1, 0:1] + 1.0) / jnp.sqrt(sums[1:2, 0:1] + 1.0)
    step = scale * own_update[...]
    step_v[...] = step
    nw_v[...] = w_v[...] - step_size * step
    take(6)
    take(7)
    for oo in range(N):
        for ii in range(N):
            first = W[0, ii, oo].astype(F32) - step_size * (scale * upd[0, ii, oo])
            wc_v[ii, oo, 0] = first.astype(BF16)
            second = W[1, ii, oo].astype(F32) - step_size * (scale * upd[1, ii, oo])
            wc_v[oo, ii, 1] = second.astype(BF16)

    for n in range(3):
        x_copies[n].wait_send()
    for j in range(N):
        d2d(j).wait_send()
        settle(seven, rs1_s.at[j])
        settle(seven, g2_s.at[j])
        settle(seven, a2_s.at[j])
        settle(ar_in.at[j] if (j // 2) % 2 == 1 else seven, ar_s.at[j])

    def sent(k, _):
        settle(W.at[c, :, o], w2_s.at[k])
        return 0

    lax.fori_loop(0, N - 1, sent, 0)
    settle(seven, a1_s)
    settle(seven, w1_s)
    for sem in (g3_s, a3_s, w3_s):
        settle(W.at[c], sem)
    settle(t1.at[pl.ds(0, N - 1)], t_s.at[0])
    settle(t2.at[pl.ds(0, N - 1)], t_s.at[1])
    settle(t3, t_s.at[2])
    settle(t4.at[pl.ds(0, 3)], t_s.at[3])


def write(*refs):
    *refs, sem = refs
    stores = [pltpu.make_async_copy(refs[n], refs[5 + n], sem.at[n]) for n in (4, 2, 0, 1, 3)]
    for store in stores:
        store.start()
    for store in stores:
        store.wait()


def body(rnn_out, out_grad, weight, left_root, right_root, left_stat, right_stat):
    tokens = rnn_out.shape[0]
    hbm = pl.BlockSpec(memory_space=pl.ANY)
    vmem = pl.BlockSpec(memory_space=pltpu.VMEM)
    v = pltpu.VMEM
    dma = pltpu.SemaphoreType.DMA
    outs = (((16, 384), F32), ((16, 384), F32), ((16, 2048), F32), ((3, 1, 384), F32), ((N, N, 2, 16, 384), BF16))
    results = pl.pallas_call(
        kernel,
        name="step",
        out_shape=tuple(pltpu.VMEM(*shape) for shape in outs),
        in_specs=[hbm] * 7,
        out_specs=(vmem,) * 5,
        scratch_shapes=[
            v((tokens, 384), BF16), v((tokens, 384), BF16), v((tokens, 512), BF16), v((2, tokens, 256), BF16),
            v((16, 384), F32), v((16, 2048), BF16), v((384, 384), BF16), v((16, 2048), F32), v((3, 1, 384), F32),
            v((N, 2, N, 16, 384), F32), v((N, N, 16, 384), F32),
            v((N, N, 16, 384), BF16), v((N, N - 1, 16, 384), BF16),
            v((N, 16, 384), BF16), v((N, N, 16, 384), BF16),
            v((4, 2, 2, N, 16, 384), BF16), v((2, N, N, 16, 384), BF16), v((2, N, N, 16, 384), BF16),
            v((2, N, N, 16, 384), F32), v((16, 384), F32), v((16, 384), F32),
            v((N, 8, 128), F32), v((N, 8, 128), F32), v((8, 128), F32), v((8, 128), F32), v((4, 8, 128), F32),
            dma((7,)),
            dma((3,)), dma((3,)), dma((N,)), dma((N,)), dma((N,)), dma((N,)), dma((N,)), dma((N,)),
            dma((N,)), dma((N,)), dma, dma, dma, dma((N,)), dma((N,)), dma((N,)), dma, dma((N,)),
            dma, dma, dma((N - 1,)), dma((N - 1,)), dma, dma, dma((4,)), dma((4,)),
        ],
        compiler_params=pltpu.CompilerParams(collective_id=0, has_side_effects=True),
    )(rnn_out, out_grad, weight, left_root[0], right_root[0], left_stat[0], jnp.transpose(right_stat, (1, 0, 2)))
    new_weight, step, left_new, right_new, copy = pl.pallas_call(
        write,
        name="write",
        out_shape=tuple(jax.ShapeDtypeStruct(*shape) for shape in outs),
        in_specs=[vmem] * 5,
        out_specs=(hbm,) * 5,
        scratch_shapes=[dma((5,))],
    )(*(pltpu.with_memory_space_constraint(result, pltpu.VMEM) for result in results))
    return new_weight, step, left_new[None], jnp.transpose(right_new, (1, 0, 2)), copy.reshape(2048, 384)


def solution(mesh):
    torus = Mesh(mesh.devices.reshape(N, N, 2, mesh.shape["tp"]), ("fs_0", "fs_1", "fs_2", "tp"))
    return jax.shard_map(
        body,
        mesh=torus,
        in_specs=(
            P(FS, "tp"),
            P(FS, "tp"),
            P(FS, "tp"),
            P("tp", FS, None),
            P("tp", None, None),
            P("tp", FS, None),
            P("tp", FS, None),
        ),
        out_specs=(P(FS, "tp"), P(FS, "tp"), P("tp", FS, None), P("tp", FS, None), P(None, "tp")),
        check_vma=False,
    )
```

```python
import functools

import jax
import jax.numpy as jnp
from jax import lax
from jax.experimental import pallas as pl
from jax.experimental.pallas import tpu as pltpu
from jax.sharding import Mesh
from jax.sharding import PartitionSpec as P

FS = ("fs_0", "fs_1", "fs_2")
MESH = pl.DeviceIdType.MESH
N = 8
F32 = jnp.float32
BF16 = jnp.bfloat16

decay_rate = 0.8
step_size = 0.005


LAST = (5, 7)
FAR_FIRST = (4, 5, 3, 6, 2, 7, 1)


def kernel(
    rnn_hbm, cot_hbm, w_hbm, lroot_hbm, rroot_hbm, lstat_hbm, rstat_hbm,
    nw_v, step_v, left_v, right_v, wc_v,
    rnn_own, rnn_in, cot_own, cot_in, w_v, lroot, rroot, lstat, rstat,
    part, part_in, rs1_out, rs1_in, ar_out, ar_in, G, A, W, upd, own_update, piece_v, t1, t2, t3,
    load_sem, known,
    x_s, x_r, d2d_s, d2d_r, rs1_s, rs1_r, ar_s, ar_r,
    g2_s, g2_r, g2_up, g2_down, g3_s, g3_r, a1_s, a1_r, a2_s, a2_r, a2_up, a2_down, a3_s, a3_r,
    w1_s, w1_r, w2_s, w2_r, w3_s, w3_r, t_s, t_r,
):
    z, y, c, x = (lax.axis_index(a) for a in ("fs_0", "fs_1", "fs_2", "tp"))
    rem = lax.rem
    o = y + c * (z - y)
    i = z + c * (y - z)
    x_rnn = x + 1 - 2 * rem(x, 2)
    x_cot = 3 - x
    blocks = (x, x_rnn, x_cot, rem(x + 2, 4))

    def outer(k):
        return (rem(z + c * k, N), rem(y + (1 - c) * k, N), c, x)

    def inner(k, xx=None):
        return (rem(z + (1 - c) * k, N), rem(y + c * k, N), c, x if xx is None else xx)

    def chip_x(k):
        return (z, y, rem(c + k // 4, 2), rem(x + k, 4))

    partner = (z, y, 1 - c, x)

    def remote(src, dst, s, r, to):
        return pltpu.make_async_remote_copy(
            src_ref=src, dst_ref=dst, send_sem=s, recv_sem=r, device_id=to, device_id_type=MESH
        )

    def settle(ref, sem):
        pltpu.make_async_copy(ref, ref, sem).wait()

    def to_all(ref, s, r, peers, order=FAR_FIRST):
        for k in order:
            remote(ref, ref, s, r, peers(k)).start()

    seven = rs1_in.at[0]
    five = rs1_in.at[0, pl.ds(0, 5)]
    def spread(at, s, r, up, down):
        for k, sem in ((2, up), (N - 2, down), (1, r(1)), (N - 1, r(N - 1))):
            remote(at(o), at(o), s, sem, outer(k)).start()

    def relay(at, s, r, up, down, four_up):
        for away, sem in ((N - 2, up), (2, down)):
            ref = at(rem(o + away, N))
            settle(ref, sem)
            turn = N - away
            if four_up == (away == N - 2):
                remote(ref, ref, s, r(4), outer(turn)).start()
            remote(ref, ref, s, r(3 if turn == 2 else 5), outer(1 if turn == 2 else N - 1)).start()

    loads = [
        pltpu.make_async_copy(src, dst, load_sem.at[n])
        for n, (src, dst) in enumerate(
            [(cot_hbm, cot_own), (rnn_hbm, rnn_own), (w_hbm, w_v), (rroot_hbm, rroot), (lroot_hbm, lroot),
             (lstat_hbm, lstat), (rstat_hbm, rstat)]
        )
    ]
    for load in loads:
        load.start()

    barrier = pltpu.get_barrier_semaphore()
    near_by = (outer(1), outer(N - 1), inner(1), inner(N - 1))
    for to in ((z, y, c, x_cot), (z, y, c, x_rnn), partner) + near_by:
        pl.semaphore_signal(barrier, inc=1, device_id=to, device_id_type=MESH)
    pl.semaphore_wait(barrier, 7)

    def learn(n, devices):
        for to in devices:
            pl.semaphore_signal(known.at[n], inc=1, device_id=to, device_id_type=MESH)

    def learned(n, count):
        pl.semaphore_wait(known.at[n], count)

    x_copies = []
    loads[0].wait()
    for h in range(2):
        cols = pl.ds(256 * h, 256)
        x_copies.append(remote(cot_own.at[:, cols], cot_in.at[h], x_s.at[h], x_r.at[h], (z, y, c, x_cot)))
    loads[1].wait()
    x_copies.append(remote(rnn_own, rnn_in, x_s.at[2], x_r.at[2], (z, y, c, x_rnn)))
    for n in (0, 2, 1):
        x_copies[n].start()
    learn(0, near_by)

    def weight_1():
        loads[2].wait()
        W[c, i, o] = w_v[...].astype(BF16)
        to_all(W.at[c, i, o], w1_s, w1_r, inner)

    def weight_2(n):
        def go(ref, up):
            remote(ref, ref, w2_s, w2_r.at[up, n], outer(1 if up else N - 1)).start()

        if n == 0:
            settle(seven, w1_r)
            go(W.at[c, :, o], 1)
            go(W.at[c, :, o], 0)
            return
        below, above = W.at[c, :, rem(o + N - n, N)], W.at[c, :, rem(o + n, N)]
        settle(below, w2_r.at[1, n - 1])
        if n < 4:
            go(below, 1)
            settle(above, w2_r.at[0, n - 1])
        if n < 3:
            go(above, 0)

    def weight_3():
        remote(W.at[c], W.at[c], w3_s, w3_r, partner).start()

    def product(cot, rnn):
        return lax.dot_general(cot, rnn, (((0,), (0,)), ((), ())), preferred_element_type=F32)

    def d2d(j):
        return remote(part.at[j, 1 - c], part_in.at[j], d2d_s.at[j], d2d_r.at[j], partner)

    def compute(j):
        q, h = j // 2, j % 2
        cot = cot_own[:, 256 * h:256 * h + 256] if q < 2 else cot_in[h]
        rnn = rnn_own[...] if q % 2 == 0 else rnn_in[...]
        part[j] = product(cot, rnn).reshape(2, N, 16, 384)
        d2d(j).start()

    def scatter_1(j):
        d2d(j).wait_recv()
        both = part[j, c] + part_in[j]
        part_in[j] = both
        rs1_out[j] = both.astype(BF16)

        for k in FAR_FIRST:
            remote(rs1_out.at[j, rem(o + k, N)], rs1_in.at[j, k - 1], rs1_s.at[j], rs1_r.at[j], outer(k)).start()

    def scatter_2(j):
        settle(seven, rs1_r.at[j])
        total = part_in[j, o]
        for k in range(N - 1):
            total = total + rs1_in[j, k].astype(F32)
        mine = total.astype(BF16)
        if (j // 2) % 2 == 1:
            ar_out[j] = mine
            for k in FAR_FIRST + (0,):
                remote(ar_out.at[j], ar_in.at[j, i], ar_s.at[j], ar_r.at[j], inner(k, x_rnn)).start()
        else:
            ar_in[j, i] = mine
            to_all(ar_in.at[j, i], ar_s.at[j], ar_r.at[j], inner)

    def g_sems(j):
        return (
            lambda s: G.at[blocks[j // 2], j % 2, c, s], g2_s.at[j], lambda k: g2_r.at[j], g2_up.at[j], g2_down.at[j]
        )

    def gather_1(j):
        settle(ar_in.at[j] if (j // 2) % 2 == 1 else seven, ar_r.at[j])
        piece = ar_in[j, 0].astype(F32)
        for s in range(1, N):
            piece = piece + ar_in[j, s].astype(F32)
        G[blocks[j // 2], j % 2, c, o] = piece.astype(BF16)

        @pl.when(i == j)
        def _():
            piece_v[...] = piece

        if j in LAST:
            to_all(G.at[blocks[j // 2], j % 2, c, o], g2_s.at[j], g2_r.at[j], outer)
        else:
            spread(*g_sems(j))

    def gather_2(j):
        relay(*g_sems(j), j % 2 == 0)

    def gather_3(j):
        settle(seven if j in LAST else five, g2_r.at[j])
        both = G.at[blocks[j // 2], j % 2, c]
        remote(both, both, g3_s, g3_r, partner).start()

    compute(0)
    compute(1)
    learned(0, 4)
    learn(1, (outer(2), outer(N - 2), inner(2), inner(N - 2)))
    learned(1, 4)
    learn(2, ((z, y, c, x_rnn),))
    weight_1()
    scatter_1(0)
    scatter_1(1)
    learned(2, 1)
    learn(3, (partner,))
    weight_2(0)
    x_copies[0].wait_recv()
    compute(4)
    scatter_2(0)
    scatter_2(1)
    scatter_1(4)
    weight_2(1)
    x_copies[2].wait_recv()
    compute(2)
    compute(3)
    compute(6)
    scatter_1(2)
    scatter_1(3)
    scatter_1(6)
    learned(3, 1)
    x_copies[1].wait_recv()
    compute(5)
    compute(7)
    gather_1(0)
    gather_1(1)
    scatter_1(5)
    scatter_1(7)
    scatter_2(4)
    weight_2(2)
    gather_2(0)
    gather_2(1)
    scatter_2(2)
    scatter_2(3)
    scatter_2(6)
    gather_1(4)
    scatter_2(5)
    scatter_2(7)
    gather_1(2)
    gather_1(3)
    gather_1(6)
    gather_2(4)
    gather_3(0)
    gather_3(1)
    gather_1(5)
    gather_1(7)
    gather_2(2)
    gather_2(3)
    gather_2(6)
    weight_2(3)
    gather_3(4)
    gather_3(2)
    gather_3(3)
    gather_3(6)
    gather_3(5)
    gather_3(7)
    for n in range(3, 7):
        loads[n].wait()
    settle(W.at[0], g3_r)

    grad = G[...].reshape(2048, 384)
    rows = jnp.dot(lroot[...], grad, preferred_element_type=F32).astype(BF16)
    A[c, i, o] = rows
    to_all(A.at[c, i, o], a1_s, a1_r.at[i], inner)

    def a_sems(n):
        half = (n + 1) // 2
        j = rem(i + half + ((n + 1) % 2) * (N - 2 * half), N)
        return lambda s: A.at[c, j, s], a2_s, lambda k: a2_r.at[k], a2_up.at[j], a2_down.at[j], a1_r.at[j]

    def applied_2(n):
        *sems, arrival = a_sems(n)
        if n:
            settle(sems[0](o), arrival)
        spread(sems[0], sems[1].at[0], *sems[2:])

    def applied_3(n):
        at, s, *sems, _ = a_sems(n)
        relay(at, s.at[0], *sems, n % 2 == 0)

    applied_2(0)

    update = jnp.dot(rows, rroot[...], preferred_element_type=F32)
    own_update[...] = update
    line = lax.broadcasted_iota(jnp.int32, (8, 128), 0)
    t1[o] = jnp.where(line == 0, jnp.sum(piece_v[...] * piece_v[...]), jnp.sum(update * update))
    to_all(t1.at[o], t_s.at[0], t_r.at[0], outer)

    applied_2(1)
    applied_2(2)
    applied_3(0)
    for n in range(3, N):
        applied_2(n)

    def total_of(ref, count):
        total = ref[0]
        for s in range(1, count):
            total = total + ref[s]
        return total

    settle(t1.at[pl.ds(0, N - 1)], t_r.at[0])
    t2[i] = total_of(t1, N)
    to_all(t2.at[i], t_s.at[1], t_r.at[1], inner)

    index = (z * N + y) * 2 + c
    own = G[z // 2, rem(z, 2), y // 4, rem(y, 4) * 2 + c]
    outer_sum = lax.dot_general(own, grad, (((1,), (1,)), ((), ())), preferred_element_type=F32)
    left_v[...] = decay_rate * lstat[...] + (1.0 - decay_rate) * (outer_sum / 384)
    pick_row = lax.broadcasted_iota(jnp.int32, (16, 384), 0)
    pick_col = lax.broadcasted_iota(jnp.int32, (16, 384), 1)
    pick = jnp.where((pick_col == 3 * index + pick_row) & (pick_row < 3), 1.0, 0.0).astype(BF16)
    columns = lax.dot_general(pick, grad, (((1,), (1,)), ((), ())), preferred_element_type=F32).astype(BF16)
    right_sum = jnp.dot(columns, grad, preferred_element_type=F32)
    for r in range(3):
        right_v[r] = decay_rate * rstat[r] + (1.0 - decay_rate) * (right_sum[r:r + 1] / 2048)

    weight_2(4)
    for n in range(1, N):
        applied_3(n)
    remote(A.at[c, :, o], A.at[c, :, o], a3_s, a3_r.at[0], partner).start()

    weight_3()

    def multiply(core, rows_of):
        for s in rows_of:
            upd[core, :, s] = jnp.dot(
                A[core, :, s].reshape(128, 384), rroot[...], preferred_element_type=F32
            ).reshape(N, 16, 384)

    def source(k):
        return rem(o - k + N, N)

    def partner_source(k):
        return rem(i - k + N, N)

    def pass_on(k):
        s = source(k)
        if k not in (2, N - 2):
            settle(A.at[c, :, s], a2_r.at[k])
        remote(A.at[c, :, s], A.at[c, :, s], a3_s, a3_r.at[k], partner).start()

    def take(k):
        settle(A.at[1 - c, :, partner_source(k)], a3_r.at[k])

    def finish(core, rows_of):
        for s in rows_of:
            for t in range(N):
                value = W[core, t, s].astype(F32) - step_size * (scale * upd[core, t, s])
                wc_v[t + core * (s - t), s + core * (t - s), core] = value.astype(BF16)

    early, late = (0, 2, 6, 1, 7), (3, 5, 4)
    pass_on(2)
    pass_on(6)
    settle(t2.at[pl.ds(0, N - 1)], t_r.at[1])
    t3[c, x] = total_of(t2, N)
    to_all(t3.at[c, x], t_s.at[2], t_r.at[2], chip_x)
    pass_on(1)
    pass_on(7)
    multiply(c, [source(k) for k in early])
    for k in early:
        take(k)
    multiply(1 - c, [partner_source(k) for k in early])
    for k in late:
        pass_on(k)
    multiply(c, [source(k) for k in late])
    settle(W.at[1 - c], w3_r)
    settle(t1.at[pl.ds(0, N - 1)], t_r.at[2])
    sums = total_of(t3[0] + t3[1], 4)
    scale = jnp.sqrt(sums[0:1, 0:1] + 1.0) / jnp.sqrt(sums[1:2, 0:1] + 1.0)
    step = scale * own_update[...]
    step_v[...] = step
    nw_v[...] = w_v[...] - step_size * step
    finish(c, [source(k) for k in early + late])
    finish(1 - c, [partner_source(k) for k in early])
    for k in late:
        take(k)
    multiply(1 - c, [partner_source(k) for k in late])
    finish(1 - c, [partner_source(k) for k in late])

    for n in range(3):
        x_copies[n].wait_send()
    for j in range(N):
        d2d(j).wait_send()
        settle(seven, rs1_s.at[j])
        settle(seven, g2_s.at[j])
        settle(ar_in.at[j] if (j // 2) % 2 == 1 else seven, ar_s.at[j])

    settle(W.at[c, :, pl.ds(0, N - 1)], w2_s)
    settle(seven, a1_s)
    settle(A.at[c, pl.ds(0, N - 1)], a2_s.at[0])
    settle(seven, w1_s)
    for sem in (g3_s, a3_s, w3_s):
        settle(W.at[c], sem)
    settle(t1.at[pl.ds(0, N - 1)], t_s.at[0])
    settle(t2.at[pl.ds(0, N - 1)], t_s.at[1])
    settle(t1.at[pl.ds(0, N - 1)], t_s.at[2])


def write(*refs):
    *refs, sem = refs
    stores = [pltpu.make_async_copy(refs[n], refs[5 + n], sem.at[n]) for n in (4, 2, 0, 1, 3)]
    for store in stores:
        store.start()
    for store in stores:
        store.wait()


def body(rnn_out, out_grad, weight, left_root, right_root, left_stat, right_stat):
    tokens = rnn_out.shape[0]
    hbm = pl.BlockSpec(memory_space=pl.ANY)
    vmem = pl.BlockSpec(memory_space=pltpu.VMEM)
    v = pltpu.VMEM
    dma = pltpu.SemaphoreType.DMA
    outs = (((16, 384), F32), ((16, 384), F32), ((16, 2048), F32), ((3, 1, 384), F32), ((N, N, 2, 16, 384), BF16))
    results = pl.pallas_call(
        kernel,
        name="step",
        out_shape=tuple(pltpu.VMEM(*shape) for shape in outs),
        in_specs=[hbm] * 7,
        out_specs=(vmem,) * 5,
        scratch_shapes=[
            v((tokens, 384), BF16), v((tokens, 384), BF16), v((tokens, 512), BF16), v((2, tokens, 256), BF16),
            v((16, 384), F32), v((16, 2048), BF16), v((384, 384), BF16), v((16, 2048), F32), v((3, 1, 384), F32),
            v((N, 2, N, 16, 384), F32), v((N, N, 16, 384), F32),
            v((N, N, 16, 384), BF16), v((N, N - 1, 16, 384), BF16),
            v((N, 16, 384), BF16), v((N, N, 16, 384), BF16),
            v((4, 2, 2, N, 16, 384), BF16), v((2, N, N, 16, 384), BF16), v((2, N, N, 16, 384), BF16),
            v((2, N, N, 16, 384), F32), v((16, 384), F32), v((16, 384), F32),
            v((N, 8, 128), F32), v((N, 8, 128), F32), v((2, 4, 8, 128), F32),
            dma((7,)), pltpu.SemaphoreType.REGULAR((4,)),
            dma((3,)), dma((3,)), dma((N,)), dma((N,)), dma((N,)), dma((N,)), dma((N,)), dma((N,)),
            dma((N,)), dma((N,)), dma((N,)), dma((N,)), dma, dma,
            dma, dma((N,)), dma((N,)), dma((N,)), dma((N,)), dma((N,)), dma, dma((N,)),
            dma, dma, dma, dma((2, 4)), dma, dma, dma((3,)), dma((3,)),
        ],
        compiler_params=pltpu.CompilerParams(collective_id=0, has_side_effects=True),
    )(rnn_out, out_grad, weight, left_root[0], right_root[0], left_stat[0], jnp.transpose(right_stat, (1, 0, 2)))
    new_weight, step, left_new, right_new, copy = pl.pallas_call(
        write,
        name="write",
        out_shape=tuple(jax.ShapeDtypeStruct(*shape) for shape in outs),
        in_specs=[vmem] * 5,
        out_specs=(hbm,) * 5,
        scratch_shapes=[dma((5,))],
    )(*(pltpu.with_memory_space_constraint(result, pltpu.VMEM) for result in results))
    return new_weight, step, left_new[None], jnp.transpose(right_new, (1, 0, 2)), copy.reshape(2048, 384)


def solution(mesh):
    torus = Mesh(mesh.devices.reshape(N, N, 2, mesh.shape["tp"]), ("fs_0", "fs_1", "fs_2", "tp"))
    return jax.shard_map(
        body,
        mesh=torus,
        in_specs=(
            P(FS, "tp"),
            P(FS, "tp"),
            P(FS, "tp"),
            P("tp", FS, None),
            P("tp", None, None),
            P("tp", FS, None),
            P("tp", FS, None),
        ),
        out_specs=(P(FS, "tp"), P(FS, "tp"), P("tp", FS, None), P("tp", FS, None), P(None, "tp")),
        check_vma=False,
    )
```

```python
import functools

import jax
import jax.numpy as jnp
from jax import lax
from jax.experimental import pallas as pl
from jax.experimental.pallas import tpu as pltpu
from jax.sharding import Mesh
from jax.sharding import PartitionSpec as P

FS = ("fs_0", "fs_1", "fs_2")
MESH = pl.DeviceIdType.MESH
N = 8
F32 = jnp.float32
BF16 = jnp.bfloat16

decay_rate = 0.8
step_size = 0.005


LAST = (5, 7)
RELAYED = 8
FAR_FIRST = (4, 5, 3, 6, 2, 7, 1)


def kernel(
    rnn_hbm, cot_hbm, w_hbm, lroot_hbm, rroot_hbm, lstat_hbm, rstat_hbm,
    nw_v, step_v, left_v, right_v, wc_v,
    rnn_own, rnn_in, cot_own, cot_in, w_v, lroot, rroot, lstat, rstat,
    part, part_in, rs1_out, rs1_in, ar_out, ar_in, G, A, W, upd, own_update, piece_v, t1, t2, t3,
    load_sem, known,
    x_s, x_r, d2d_s, d2d_r, rs1_s, rs1_r, ar_s, ar_r,
    g2_s, g2_r, g2_up, g2_down, g3_s, g3_r, a1_s, a1_r, a2_s, a2_r, a2_up, a2_down, a3_s, a3_r,
    w1_s, w1_r, w2_s, w2_r, w3_s, w3_r, t_s, t_r,
):
    z, y, c, x = (lax.axis_index(a) for a in ("fs_0", "fs_1", "fs_2", "tp"))
    rem = lax.rem
    o = y + c * (z - y)
    i = z + c * (y - z)
    x_rnn = x + 1 - 2 * rem(x, 2)
    x_cot = 3 - x
    blocks = (x, x_rnn, x_cot, rem(x + 2, 4))

    def outer(k):
        return (rem(z + c * k, N), rem(y + (1 - c) * k, N), c, x)

    def inner(k, xx=None):
        return (rem(z + (1 - c) * k, N), rem(y + c * k, N), c, x if xx is None else xx)

    partner = (z, y, 1 - c, x)

    def remote(src, dst, s, r, to):
        return pltpu.make_async_remote_copy(
            src_ref=src, dst_ref=dst, send_sem=s, recv_sem=r, device_id=to, device_id_type=MESH
        )

    def settle(ref, sem):
        pltpu.make_async_copy(ref, ref, sem).wait()

    def to_all(ref, s, r, peers, order=FAR_FIRST):
        for k in order:
            remote(ref, ref, s, r, peers(k)).start()

    seven = rs1_in.at[0]
    five = rs1_in.at[0, pl.ds(0, 5)]
    thirty_one = t2.at[pl.ds(0, 4 * N - 1)]
    def spread(at, s, r, up, down):
        for k, sem in ((2, up), (N - 2, down), (1, r(1)), (N - 1, r(N - 1))):
            remote(at(o), at(o), s, sem, outer(k)).start()

    def relay(at, s, r, up, down, four_up):
        for away, sem in ((N - 2, up), (2, down)):
            ref = at(rem(o + away, N))
            settle(ref, sem)
            turn = N - away
            if four_up == (away == N - 2):
                remote(ref, ref, s, r(4), outer(turn)).start()
            remote(ref, ref, s, r(3 if turn == 2 else 5), outer(1 if turn == 2 else N - 1)).start()

    loads = [
        pltpu.make_async_copy(src, dst, load_sem.at[n])
        for n, (src, dst) in enumerate(
            [(cot_hbm, cot_own), (rnn_hbm, rnn_own), (w_hbm, w_v), (rroot_hbm, rroot), (lroot_hbm, lroot),
             (lstat_hbm, lstat), (rstat_hbm, rstat)]
        )
    ]
    for load in loads:
        load.start()

    barrier = pltpu.get_barrier_semaphore()
    near_by = (outer(1), outer(N - 1), inner(1), inner(N - 1))
    for to in ((z, y, c, x_cot), (z, y, c, x_rnn), partner) + near_by:
        pl.semaphore_signal(barrier, inc=1, device_id=to, device_id_type=MESH)
    pl.semaphore_wait(barrier, 7)

    def learn(n, devices):
        for to in devices:
            pl.semaphore_signal(known.at[n], inc=1, device_id=to, device_id_type=MESH)

    def learned(n, count):
        pl.semaphore_wait(known.at[n], count)

    x_copies = []
    loads[0].wait()
    for h in range(2):
        cols = pl.ds(256 * h, 256)
        x_copies.append(remote(cot_own.at[:, cols], cot_in.at[h], x_s.at[h], x_r.at[h], (z, y, c, x_cot)))
    loads[1].wait()
    x_copies.append(remote(rnn_own, rnn_in, x_s.at[2], x_r.at[2], (z, y, c, x_rnn)))
    for n in (0, 2, 1):
        x_copies[n].start()
    learn(0, near_by)

    def weight_1():
        loads[2].wait()
        W[c, i, o] = w_v[...].astype(BF16)
        to_all(W.at[c, i, o], w1_s, w1_r, inner)

    def weight_2(n):
        def go(ref, up):
            remote(ref, ref, w2_s, w2_r.at[up, n], outer(1 if up else N - 1)).start()

        if n == 0:
            settle(seven, w1_r)
            go(W.at[c, :, o], 1)
            go(W.at[c, :, o], 0)
            return
        below, above = W.at[c, :, rem(o + N - n, N)], W.at[c, :, rem(o + n, N)]
        settle(below, w2_r.at[1, n - 1])
        if n < 4:
            go(below, 1)
            settle(above, w2_r.at[0, n - 1])
        if n < 3:
            go(above, 0)

    def weight_3():
        remote(W.at[c], W.at[c], w3_s, w3_r, partner).start()

    def product(cot, rnn):
        return lax.dot_general(cot, rnn, (((0,), (0,)), ((), ())), preferred_element_type=F32)

    def d2d(j):
        return remote(part.at[j, 1 - c], part_in.at[j], d2d_s.at[j], d2d_r.at[j], partner)

    def compute(j):
        q, h = j // 2, j % 2
        cot = cot_own[:, 256 * h:256 * h + 256] if q < 2 else cot_in[h]
        rnn = rnn_own[...] if q % 2 == 0 else rnn_in[...]
        part[j] = product(cot, rnn).reshape(2, N, 16, 384)
        d2d(j).start()

    def scatter_1(j):
        d2d(j).wait_recv()
        both = part[j, c] + part_in[j]
        part_in[j] = both
        rs1_out[j] = both.astype(BF16)

        for k in FAR_FIRST:
            remote(rs1_out.at[j, rem(o + k, N)], rs1_in.at[j, k - 1], rs1_s.at[j], rs1_r.at[j], outer(k)).start()

    def scatter_2(j):
        settle(seven, rs1_r.at[j])
        total = part_in[j, o]
        for k in range(N - 1):
            total = total + rs1_in[j, k].astype(F32)
        mine = total.astype(BF16)
        if (j // 2) % 2 == 1:
            ar_out[j] = mine
            for k in FAR_FIRST + (0,):
                remote(ar_out.at[j], ar_in.at[j, i], ar_s.at[j], ar_r.at[j], inner(k, x_rnn)).start()
        else:
            ar_in[j, i] = mine
            to_all(ar_in.at[j, i], ar_s.at[j], ar_r.at[j], inner)

    def g_sems(j):
        return (
            lambda s: G.at[blocks[j // 2], j % 2, c, s], g2_s.at[j], lambda k: g2_r.at[j], g2_up.at[j], g2_down.at[j]
        )

    def gather_1(j):
        settle(ar_in.at[j] if (j // 2) % 2 == 1 else seven, ar_r.at[j])
        piece = ar_in[j, 0].astype(F32)
        for s in range(1, N):
            piece = piece + ar_in[j, s].astype(F32)
        G[blocks[j // 2], j % 2, c, o] = piece.astype(BF16)

        @pl.when(i == j)
        def _():
            piece_v[...] = piece

        if j in LAST:
            to_all(G.at[blocks[j // 2], j % 2, c, o], g2_s.at[j], g2_r.at[j], outer)
        else:
            spread(*g_sems(j))

    def gather_2(j):
        relay(*g_sems(j), j % 2 == 0)

    def gather_3(j):
        settle(seven if j in LAST else five, g2_r.at[j])
        both = G.at[blocks[j // 2], j % 2, c]
        remote(both, both, g3_s, g3_r, partner).start()

    compute(0)
    compute(1)
    learned(0, 4)
    learn(1, (outer(2), outer(N - 2), inner(2), inner(N - 2)))
    learned(1, 4)
    learn(2, ((z, y, c, x_rnn), (z, y, c, x_cot)))
    weight_1()
    scatter_1(0)
    scatter_1(1)
    learned(2, 2)
    learn(3, ((z, y, c, x_rnn), partner))
    weight_2(0)
    x_copies[0].wait_recv()
    compute(4)
    scatter_2(0)
    scatter_2(1)
    scatter_1(4)
    weight_2(1)
    x_copies[2].wait_recv()
    compute(2)
    compute(3)
    compute(6)
    scatter_1(2)
    scatter_1(3)
    scatter_1(6)
    learned(3, 2)
    x_copies[1].wait_recv()
    compute(5)
    compute(7)
    gather_1(0)
    gather_1(1)
    scatter_1(5)
    scatter_1(7)
    scatter_2(4)
    weight_2(2)
    scatter_2(2)
    scatter_2(3)
    scatter_2(6)
    gather_2(0)
    gather_2(1)
    gather_1(4)
    scatter_2(5)
    scatter_2(7)
    gather_1(2)
    gather_1(3)
    gather_1(6)
    gather_2(4)
    gather_3(0)
    gather_3(1)
    gather_1(5)
    gather_1(7)
    gather_2(2)
    gather_2(3)
    gather_2(6)
    weight_2(3)
    gather_3(4)
    gather_3(2)
    gather_3(3)
    gather_3(6)
    gather_3(5)
    gather_3(7)
    for n in range(3, 7):
        loads[n].wait()
    settle(W.at[0], g3_r)

    grad = G[...].reshape(2048, 384)
    rows = jnp.dot(lroot[...], grad, preferred_element_type=F32).astype(BF16)
    A[c, i, o] = rows
    to_all(A.at[c, i, o], a1_s, a1_r.at[i], inner)

    def a_sems(n):
        half = (n + 1) // 2
        j = rem(i + half + ((n + 1) % 2) * (N - 2 * half), N)
        return lambda s: A.at[c, j, s], a2_s, lambda k: a2_r.at[k], a2_up.at[j], a2_down.at[j], a1_r.at[j]

    def applied_2(n):
        *sems, arrival = a_sems(n)
        if n:
            settle(sems[0](o), arrival)
        if n < RELAYED:
            spread(sems[0], sems[1].at[0], *sems[2:])
        else:
            at, s, r, up, down = sems
            for k in FAR_FIRST:
                sem = {2: up, N - 2: down}.get(k)
                remote(at(o), at(o), s.at[0], r(k) if sem is None else sem, outer(k)).start()

    def applied_3(n):
        at, s, *sems, _ = a_sems(n)
        if n < RELAYED:
            relay(at, s.at[0], *sems, n % 2 == 0)
        else:
            settle(at(rem(o + N - 2, N)), sems[1])
            settle(at(rem(o + 2, N)), sems[2])

    applied_2(0)

    update = jnp.dot(rows, rroot[...], preferred_element_type=F32)
    own_update[...] = update
    lane = lax.broadcasted_iota(jnp.int32, (1, 128), 1)
    t1[o] = jnp.where(lane == 0, jnp.sum(piece_v[...] * piece_v[...]), jnp.sum(update * update))
    to_all(t1.at[o], t_s.at[0], t_r.at[0], outer)
    weight_2(4)
    weight_3()

    applied_2(1)
    applied_2(2)
    applied_3(0)
    for n in range(3, N):
        applied_2(n)

    def total_of(ref, count):
        total = ref[0]
        for s in range(1, count):
            total = total + ref[s]
        return total

    settle(t1.at[pl.ds(0, N - 1)], t_r.at[0])
    mine = N * x + i
    t2[mine] = total_of(t1, N)
    for k in FAR_FIRST:
        for away in (2, 1, 3, 0):
            remote(t2.at[mine], t2.at[mine], t_s.at[1], t_r.at[1], inner(k, rem(x + away, 4))).start()
    for away in (2, 1, 3):
        remote(t2.at[mine], t2.at[mine], t_s.at[1], t_r.at[1], (z, y, c, rem(x + away, 4))).start()

    index = (z * N + y) * 2 + c
    own = G[z // 2, rem(z, 2), y // 4, rem(y, 4) * 2 + c]
    outer_sum = lax.dot_general(own, grad, (((1,), (1,)), ((), ())), preferred_element_type=F32)
    left_v[...] = decay_rate * lstat[...] + (1.0 - decay_rate) * (outer_sum / 384)
    pick_row = lax.broadcasted_iota(jnp.int32, (16, 384), 0)
    pick_col = lax.broadcasted_iota(jnp.int32, (16, 384), 1)
    pick = jnp.where((pick_col == 3 * index + pick_row) & (pick_row < 3), 1.0, 0.0).astype(BF16)
    columns = lax.dot_general(pick, grad, (((1,), (1,)), ((), ())), preferred_element_type=F32).astype(BF16)
    right_sum = jnp.dot(columns, grad, preferred_element_type=F32)
    for r in range(3):
        right_v[r] = decay_rate * rstat[r] + (1.0 - decay_rate) * (right_sum[r:r + 1] / 2048)

    for n in range(1, N):
        applied_3(n)
    remote(A.at[c, :, o], A.at[c, :, o], a3_s, a3_r.at[0], partner).start()

    def multiply(core, rows_of):
        for s in rows_of:
            upd[core, :, s] = jnp.dot(
                A[core, :, s].reshape(128, 384), rroot[...], preferred_element_type=F32
            ).reshape(N, 16, 384)

    def source(k):
        return rem(o - k + N, N)

    def partner_source(k):
        return rem(i - k + N, N)

    def pass_on(k):
        s = source(k)
        if k not in (2, N - 2):
            settle(A.at[c, :, s], a2_r.at[k])
        remote(A.at[c, :, s], A.at[c, :, s], a3_s, a3_r.at[k], partner).start()

    def take(k):
        settle(A.at[1 - c, :, partner_source(k)], a3_r.at[k])

    def finish(core, rows_of):
        for s in rows_of:
            for t in range(N):
                value = W[core, t, s].astype(F32) - step_size * (scale * upd[core, t, s])
                wc_v[t + core * (s - t), s + core * (t - s), core] = value.astype(BF16)

    early, late = (0, 2, 6, 1, 7), (3, 5, 4)
    pass_on(2)
    pass_on(6)
    settle(thirty_one, t_r.at[1])
    t3[c] = total_of(t2, 4 * N)
    remote(t3.at[c], t3.at[c], t_s.at[2], t_r.at[2], partner).start()
    pass_on(1)
    pass_on(7)
    multiply(c, [source(k) for k in early])
    for k in early:
        take(k)
    multiply(1 - c, [partner_source(k) for k in early])
    for k in late:
        pass_on(k)
    multiply(c, [source(k) for k in late])
    settle(W.at[1 - c], w3_r)
    settle(t3.at[0], t_r.at[2])
    sums = t3[0] + t3[1]
    scale = jnp.sqrt(sums[0:1, 0:1] + 1.0) / jnp.sqrt(sums[0:1, 1:2] + 1.0)
    step = scale * own_update[...]
    step_v[...] = step
    nw_v[...] = w_v[...] - step_size * step
    finish(c, [source(k) for k in early + late])
    finish(1 - c, [partner_source(k) for k in early])
    for k in late:
        take(k)
    multiply(1 - c, [partner_source(k) for k in late])
    finish(1 - c, [partner_source(k) for k in late])

    for n in range(3):
        x_copies[n].wait_send()
    for j in range(N):
        d2d(j).wait_send()
        settle(seven, rs1_s.at[j])
        settle(seven, g2_s.at[j])
        settle(ar_in.at[j] if (j // 2) % 2 == 1 else seven, ar_s.at[j])

    settle(W.at[c, :, pl.ds(0, N - 1)], w2_s)
    settle(seven, a1_s)
    settle(A.at[c, pl.ds(0, N - 1)], a2_s.at[0])
    settle(seven, w1_s)
    for sem in (g3_s, a3_s, w3_s):
        settle(W.at[c], sem)
    settle(t1.at[pl.ds(0, N - 1)], t_s.at[0])
    settle(thirty_one, t_s.at[1])
    settle(t3.at[0], t_s.at[2])


def write(*refs):
    *refs, sem = refs
    stores = [pltpu.make_async_copy(refs[n], refs[5 + n], sem.at[n]) for n in (4, 2, 0, 1, 3)]
    for store in stores:
        store.start()
    for store in stores:
        store.wait()


def body(rnn_out, out_grad, weight, left_root, right_root, left_stat, right_stat):
    tokens = rnn_out.shape[0]
    hbm = pl.BlockSpec(memory_space=pl.ANY)
    vmem = pl.BlockSpec(memory_space=pltpu.VMEM)
    v = pltpu.VMEM
    dma = pltpu.SemaphoreType.DMA
    outs = (((16, 384), F32), ((16, 384), F32), ((16, 2048), F32), ((3, 1, 384), F32), ((N, N, 2, 16, 384), BF16))
    results = pl.pallas_call(
        kernel,
        name="step",
        out_shape=tuple(pltpu.VMEM(*shape) for shape in outs),
        in_specs=[hbm] * 7,
        out_specs=(vmem,) * 5,
        scratch_shapes=[
            v((tokens, 384), BF16), v((tokens, 384), BF16), v((tokens, 512), BF16), v((2, tokens, 256), BF16),
            v((16, 384), F32), v((16, 2048), BF16), v((384, 384), BF16), v((16, 2048), F32), v((3, 1, 384), F32),
            v((N, 2, N, 16, 384), F32), v((N, N, 16, 384), F32),
            v((N, N, 16, 384), BF16), v((N, N - 1, 16, 384), BF16),
            v((N, 16, 384), BF16), v((N, N, 16, 384), BF16),
            v((4, 2, 2, N, 16, 384), BF16), v((2, N, N, 16, 384), BF16), v((2, N, N, 16, 384), BF16),
            v((2, N, N, 16, 384), F32), v((16, 384), F32), v((16, 384), F32),
            v((N, 1, 128), F32), v((4 * N, 1, 128), F32), v((2, 1, 128), F32),
            dma((7,)), pltpu.SemaphoreType.REGULAR((4,)),
            dma((3,)), dma((3,)), dma((N,)), dma((N,)), dma((N,)), dma((N,)), dma((N,)), dma((N,)),
            dma((N,)), dma((N,)), dma((N,)), dma((N,)), dma, dma,
            dma, dma((N,)), dma((N,)), dma((N,)), dma((N,)), dma((N,)), dma, dma((N,)),
            dma, dma, dma, dma((2, 4)), dma, dma, dma((3,)), dma((3,)),
        ],
        compiler_params=pltpu.CompilerParams(collective_id=0, has_side_effects=True),
    )(rnn_out, out_grad, weight, left_root[0], right_root[0], left_stat[0], jnp.transpose(right_stat, (1, 0, 2)))
    new_weight, step, left_new, right_new, copy = pl.pallas_call(
        write,
        name="write",
        out_shape=tuple(jax.ShapeDtypeStruct(*shape) for shape in outs),
        in_specs=[vmem] * 5,
        out_specs=(hbm,) * 5,
        scratch_shapes=[dma((5,))],
    )(*(pltpu.with_memory_space_constraint(result, pltpu.VMEM) for result in results))
    return new_weight, step, left_new[None], jnp.transpose(right_new, (1, 0, 2)), copy.reshape(2048, 384)


def solution(mesh):
    torus = Mesh(mesh.devices.reshape(N, N, 2, mesh.shape["tp"]), ("fs_0", "fs_1", "fs_2", "tp"))
    return jax.shard_map(
        body,
        mesh=torus,
        in_specs=(
            P(FS, "tp"),
            P(FS, "tp"),
            P(FS, "tp"),
            P("tp", FS, None),
            P("tp", None, None),
            P("tp", FS, None),
            P("tp", FS, None),
        ),
        out_specs=(P(FS, "tp"), P(FS, "tp"), P("tp", FS, None), P("tp", FS, None), P(None, "tp")),
        check_vma=False,
    )
```

```python
import functools

import jax
import jax.numpy as jnp
from jax import lax
from jax.experimental import pallas as pl
from jax.experimental.pallas import tpu as pltpu
from jax.sharding import Mesh
from jax.sharding import PartitionSpec as P

FS = ("fs_0", "fs_1", "fs_2")
MESH = pl.DeviceIdType.MESH
N = 8
F32 = jnp.float32
BF16 = jnp.bfloat16

decay_rate = 0.8
step_size = 0.005


LAST = (5, 7)
RELAYED = 8
FAR_FIRST = (4, 5, 3, 6, 2, 7, 1)


def kernel(
    rnn_hbm, cot_hbm, w_hbm, lroot_hbm, rroot_hbm, lstat_hbm, rstat_hbm,
    nw_v, step_v, left_v, right_v, wc_v,
    rnn_own, rnn_in, cot_own, cot_in, w_v, lroot, rroot, lstat, rstat,
    part, part_in, rs1_out, rs1_in, ar_out, ar_in, G, A, W, upd, own_update, piece_v, t1, t2, t3,
    load_sem, known,
    x_s, x_r, d2d_s, d2d_r, rs1_s, rs1_r, ar_s, ar_r,
    g2_s, g2_r, g2_up, g2_down, g3_s, g3_r, a1_s, a1_r, a2_s, a2_r, a2_up, a2_down, a3_s, a3_r,
    w1_s, w1_r, w2_s, w2_r, w3_s, w3_r, t_s, t_r,
):
    z, y, c, x = (lax.axis_index(a) for a in ("fs_0", "fs_1", "fs_2", "tp"))
    rem = lax.rem
    o = y + c * (z - y)
    i = z + c * (y - z)
    x_rnn = x + 1 - 2 * rem(x, 2)
    x_cot = 3 - x
    blocks = (x, x_rnn, x_cot, rem(x + 2, 4))

    def outer(k):
        return (rem(z + c * k, N), rem(y + (1 - c) * k, N), c, x)

    def inner(k, xx=None):
        return (rem(z + (1 - c) * k, N), rem(y + c * k, N), c, x if xx is None else xx)

    partner = (z, y, 1 - c, x)

    def remote(src, dst, s, r, to):
        return pltpu.make_async_remote_copy(
            src_ref=src, dst_ref=dst, send_sem=s, recv_sem=r, device_id=to, device_id_type=MESH
        )

    def settle(ref, sem):
        pltpu.make_async_copy(ref, ref, sem).wait()

    def to_all(ref, s, r, peers, order=FAR_FIRST):
        for k in order:
            remote(ref, ref, s, r, peers(k)).start()

    seven = rs1_in.at[0]
    five = rs1_in.at[0, pl.ds(0, 5)]
    thirty_one = t2.at[pl.ds(0, 4 * N - 1)]
    def spread(at, s, r, up, down):
        for k, sem in ((2, up), (N - 2, down), (1, r(1)), (N - 1, r(N - 1))):
            remote(at(o), at(o), s, sem, outer(k)).start()

    def relay(at, s, r, up, down, four_up):
        for away, sem in ((N - 2, up), (2, down)):
            ref = at(rem(o + away, N))
            settle(ref, sem)
            turn = N - away
            if four_up == (away == N - 2):
                remote(ref, ref, s, r(4), outer(turn)).start()
            remote(ref, ref, s, r(3 if turn == 2 else 5), outer(1 if turn == 2 else N - 1)).start()

    loads = [
        pltpu.make_async_copy(src, dst, load_sem.at[n])
        for n, (src, dst) in enumerate(
            [(cot_hbm, cot_own), (rnn_hbm, rnn_own), (w_hbm, w_v), (rroot_hbm, rroot), (lroot_hbm, lroot),
             (lstat_hbm, lstat), (rstat_hbm, rstat)]
        )
    ]
    for load in loads:
        load.start()

    barrier = pltpu.get_barrier_semaphore()
    near_by = (outer(1), outer(N - 1), inner(1), inner(N - 1))
    for to in ((z, y, c, x_cot), (z, y, c, x_rnn), partner) + near_by:
        pl.semaphore_signal(barrier, inc=1, device_id=to, device_id_type=MESH)
    pl.semaphore_wait(barrier, 7)

    def learn(n, devices):
        for to in devices:
            pl.semaphore_signal(known.at[n], inc=1, device_id=to, device_id_type=MESH)

    def learned(n, count):
        pl.semaphore_wait(known.at[n], count)

    x_copies = []
    loads[0].wait()
    for h in range(2):
        cols = pl.ds(256 * h, 256)
        x_copies.append(remote(cot_own.at[:, cols], cot_in.at[h], x_s.at[h], x_r.at[h], (z, y, c, x_cot)))
    loads[1].wait()
    x_copies.append(remote(rnn_own, rnn_in, x_s.at[2], x_r.at[2], (z, y, c, x_rnn)))
    for n in (0, 2, 1):
        x_copies[n].start()
    learn(0, near_by)

    def weight_1():
        loads[2].wait()
        W[c, i, o] = w_v[...].astype(BF16)
        to_all(W.at[c, i, o], w1_s, w1_r, inner)

    def weight_2(n):
        def go(ref, up):
            remote(ref, ref, w2_s, w2_r.at[up, n], outer(1 if up else N - 1)).start()

        if n == 0:
            settle(seven, w1_r)
            go(W.at[c, :, o], 1)
            go(W.at[c, :, o], 0)
            return
        below, above = W.at[c, :, rem(o + N - n, N)], W.at[c, :, rem(o + n, N)]
        settle(below, w2_r.at[1, n - 1])
        if n < 4:
            go(below, 1)
            settle(above, w2_r.at[0, n - 1])
        if n < 3:
            go(above, 0)

    def weight_3():
        remote(W.at[c], W.at[c], w3_s, w3_r, partner).start()

    def product(cot, rnn):
        return lax.dot_general(cot, rnn, (((0,), (0,)), ((), ())), preferred_element_type=F32)

    def d2d(j):
        return remote(part.at[j, 1 - c], part_in.at[j], d2d_s.at[j], d2d_r.at[j], partner)

    def compute(j):
        q, h = j // 2, j % 2
        cot = cot_own[:, 256 * h:256 * h + 256] if q < 2 else cot_in[h]
        rnn = rnn_own[...] if q % 2 == 0 else rnn_in[...]
        part[j] = product(cot, rnn).reshape(2, N, 16, 384)
        d2d(j).start()

    def scatter_1(j):
        d2d(j).wait_recv()
        both = part[j, c] + part_in[j]
        part_in[j] = both
        rs1_out[j] = both.astype(BF16)

        for k in FAR_FIRST:
            remote(rs1_out.at[j, rem(o + k, N)], rs1_in.at[j, k - 1], rs1_s.at[j], rs1_r.at[j], outer(k)).start()

    def scatter_2(j):
        settle(seven, rs1_r.at[j])
        total = part_in[j, o]
        for k in range(N - 1):
            total = total + rs1_in[j, k].astype(F32)
        mine = total.astype(BF16)
        if (j // 2) % 2 == 1:
            ar_out[j] = mine
            for k in FAR_FIRST + (0,):
                remote(ar_out.at[j], ar_in.at[j, i], ar_s.at[j], ar_r.at[j], inner(k, x_rnn)).start()
        else:
            ar_in[j, i] = mine
            to_all(ar_in.at[j, i], ar_s.at[j], ar_r.at[j], inner)

    def g_sems(j):
        return (
            lambda s: G.at[blocks[j // 2], j % 2, c, s], g2_s.at[j], lambda k: g2_r.at[j], g2_up.at[j], g2_down.at[j]
        )

    def gather_1(j):
        settle(ar_in.at[j] if (j // 2) % 2 == 1 else seven, ar_r.at[j])
        piece = ar_in[j, 0].astype(F32)
        for s in range(1, N):
            piece = piece + ar_in[j, s].astype(F32)
        G[blocks[j // 2], j % 2, c, o] = piece.astype(BF16)

        @pl.when(i == j)
        def _():
            piece_v[...] = piece

        if j in LAST:
            to_all(G.at[blocks[j // 2], j % 2, c, o], g2_s.at[j], g2_r.at[j], outer)
        else:
            spread(*g_sems(j))

    def gather_2(j):
        relay(*g_sems(j), j % 2 == 0)

    def gather_3(j):
        settle(seven if j in LAST else five, g2_r.at[j])
        both = G.at[blocks[j // 2], j % 2, c]
        remote(both, both, g3_s, g3_r, partner).start()

    compute(0)
    compute(1)
    learned(0, 4)
    learn(1, (outer(2), outer(N - 2), inner(2), inner(N - 2)))
    learned(1, 4)
    learn(2, ((z, y, c, x_rnn), (z, y, c, x_cot)))
    weight_1()
    scatter_1(0)
    scatter_1(1)
    learned(2, 2)
    learn(3, ((z, y, c, x_rnn), partner))
    weight_2(0)
    x_copies[0].wait_recv()
    compute(4)
    scatter_2(0)
    scatter_2(1)
    scatter_1(4)
    weight_2(1)
    x_copies[2].wait_recv()
    compute(2)
    compute(3)
    compute(6)
    scatter_1(2)
    scatter_1(3)
    scatter_1(6)
    learned(3, 2)
    x_copies[1].wait_recv()
    compute(5)
    compute(7)
    gather_1(0)
    gather_1(1)
    scatter_1(5)
    scatter_1(7)
    scatter_2(4)
    weight_2(2)
    scatter_2(2)
    scatter_2(3)
    scatter_2(6)
    gather_2(0)
    gather_2(1)
    gather_1(4)
    scatter_2(5)
    scatter_2(7)
    gather_1(2)
    gather_1(3)
    gather_1(6)
    gather_2(4)
    gather_3(0)
    gather_3(1)
    gather_1(5)
    gather_1(7)
    gather_2(2)
    gather_2(3)
    gather_2(6)
    weight_2(3)
    gather_3(4)
    gather_3(2)
    gather_3(3)
    gather_3(6)
    gather_3(5)
    gather_3(7)
    for n in range(3, 7):
        loads[n].wait()
    settle(W.at[0], g3_r)

    grad = G[...].reshape(2048, 384)
    rows = jnp.dot(lroot[...], grad, preferred_element_type=F32).astype(BF16)
    A[c, i, o] = rows
    to_all(A.at[c, i, o], a1_s, a1_r.at[i], inner)

    def a_sems(n):
        half = (n + 1) // 2
        j = rem(i + half + ((n + 1) % 2) * (N - 2 * half), N)
        return lambda s: A.at[c, j, s], a2_s, lambda k: a2_r.at[k], a2_up.at[j], a2_down.at[j], a1_r.at[j]

    def applied_2(n):
        *sems, arrival = a_sems(n)
        if n:
            settle(sems[0](o), arrival)
        if n < RELAYED:
            spread(sems[0], sems[1].at[0], *sems[2:])
        else:
            at, s, r, up, down = sems
            for k in FAR_FIRST:
                sem = {2: up, N - 2: down}.get(k)
                remote(at(o), at(o), s.at[0], r(k) if sem is None else sem, outer(k)).start()

    def applied_3(n):
        at, s, *sems, _ = a_sems(n)
        if n < RELAYED:
            relay(at, s.at[0], *sems, n % 2 == 0)
        else:
            settle(at(rem(o + N - 2, N)), sems[1])
            settle(at(rem(o + 2, N)), sems[2])

    applied_2(0)

    update = jnp.dot(rows, rroot[...], preferred_element_type=F32)
    own_update[...] = update
    lane = lax.broadcasted_iota(jnp.int32, (1, 128), 1)
    t1[o] = jnp.where(lane == 0, jnp.sum(piece_v[...] * piece_v[...]), jnp.sum(update * update))
    to_all(t1.at[o], t_s.at[0], t_r.at[0], outer)
    weight_2(4)
    weight_3()

    applied_2(1)
    applied_2(2)
    applied_3(0)
    for n in range(3, N):
        applied_2(n)

    def total_of(ref, count):
        total = ref[0]
        for s in range(1, count):
            total = total + ref[s]
        return total

    settle(t1.at[pl.ds(0, N - 1)], t_r.at[0])
    mine = N * x + i
    t2[mine] = total_of(t1, N)
    for k in FAR_FIRST:
        for away in (2, 1, 3, 0):
            remote(t2.at[mine], t2.at[mine], t_s.at[1], t_r.at[1], inner(k, rem(x + away, 4))).start()
    for away in (2, 1, 3):
        remote(t2.at[mine], t2.at[mine], t_s.at[1], t_r.at[1], (z, y, c, rem(x + away, 4))).start()

    for n in range(1, N):
        applied_3(n)
    remote(A.at[c, :, o], A.at[c, :, o], a3_s, a3_r.at[0], partner).start()

    def multiply(core, rows_of):
        for s in rows_of:
            upd[core, :, s] = jnp.dot(
                A[core, :, s].reshape(128, 384), rroot[...], preferred_element_type=F32
            ).reshape(N, 16, 384)

    def source(k):
        return rem(o - k + N, N)

    def partner_source(k):
        return rem(i - k + N, N)

    def pass_on(k):
        s = source(k)
        if k not in (2, N - 2):
            settle(A.at[c, :, s], a2_r.at[k])
        remote(A.at[c, :, s], A.at[c, :, s], a3_s, a3_r.at[k], partner).start()

    def take(k):
        settle(A.at[1 - c, :, partner_source(k)], a3_r.at[k])

    def finish(core, rows_of):
        for s in rows_of:
            for t in range(N):
                value = W[core, t, s].astype(F32) - step_size * (scale * upd[core, t, s])
                wc_v[t + core * (s - t), s + core * (t - s), core] = value.astype(BF16)

    early, late = (0, 2, 6, 1, 7), (3, 5, 4)
    pass_on(2)
    pass_on(6)
    pass_on(1)
    pass_on(7)
    settle(thirty_one, t_r.at[1])
    t3[c] = total_of(t2, 4 * N)
    remote(t3.at[c], t3.at[c], t_s.at[2], t_r.at[2], partner).start()
    multiply(c, [source(k) for k in early])

    index = (z * N + y) * 2 + c
    own = G[z // 2, rem(z, 2), y // 4, rem(y, 4) * 2 + c]
    outer_sum = lax.dot_general(own, grad, (((1,), (1,)), ((), ())), preferred_element_type=F32)
    left_v[...] = decay_rate * lstat[...] + (1.0 - decay_rate) * (outer_sum / 384)
    pick_row = lax.broadcasted_iota(jnp.int32, (16, 384), 0)
    pick_col = lax.broadcasted_iota(jnp.int32, (16, 384), 1)
    pick = jnp.where((pick_col == 3 * index + pick_row) & (pick_row < 3), 1.0, 0.0).astype(BF16)
    columns = lax.dot_general(pick, grad, (((1,), (1,)), ((), ())), preferred_element_type=F32).astype(BF16)
    right_sum = jnp.dot(columns, grad, preferred_element_type=F32)
    for r in range(3):
        right_v[r] = decay_rate * rstat[r] + (1.0 - decay_rate) * (right_sum[r:r + 1] / 2048)

    for k in early:
        take(k)
    multiply(1 - c, [partner_source(k) for k in early])
    for k in late:
        pass_on(k)
    multiply(c, [source(k) for k in late])
    settle(W.at[1 - c], w3_r)
    settle(t3.at[0], t_r.at[2])
    sums = t3[0] + t3[1]
    scale = jnp.sqrt(sums[0:1, 0:1] + 1.0) / jnp.sqrt(sums[0:1, 1:2] + 1.0)
    step = scale * own_update[...]
    step_v[...] = step
    nw_v[...] = w_v[...] - step_size * step
    finish(c, [source(k) for k in early + late])
    finish(1 - c, [partner_source(k) for k in early])
    for k in late:
        take(k)
    multiply(1 - c, [partner_source(k) for k in late])
    finish(1 - c, [partner_source(k) for k in late])

    for n in range(3):
        x_copies[n].wait_send()
    for j in range(N):
        d2d(j).wait_send()
        settle(seven, rs1_s.at[j])
        settle(seven, g2_s.at[j])
        settle(ar_in.at[j] if (j // 2) % 2 == 1 else seven, ar_s.at[j])

    settle(W.at[c, :, pl.ds(0, N - 1)], w2_s)
    settle(seven, a1_s)
    settle(A.at[c, pl.ds(0, N - 1)], a2_s.at[0])
    settle(seven, w1_s)
    for sem in (g3_s, a3_s, w3_s):
        settle(W.at[c], sem)
    settle(t1.at[pl.ds(0, N - 1)], t_s.at[0])
    settle(thirty_one, t_s.at[1])
    settle(t3.at[0], t_s.at[2])


def write(*refs):
    *refs, sem = refs
    pairs = [(refs[4].at[n], refs[9].at[n]) for n in range(N)] + [(refs[n], refs[5 + n]) for n in (2, 0, 1, 3)]
    stores = [pltpu.make_async_copy(src, dst, sem.at[n]) for n, (src, dst) in enumerate(pairs)]
    for store in stores:
        store.start()
    for store in stores:
        store.wait()


def body(rnn_out, out_grad, weight, left_root, right_root, left_stat, right_stat):
    tokens = rnn_out.shape[0]
    hbm = pl.BlockSpec(memory_space=pl.ANY)
    vmem = pl.BlockSpec(memory_space=pltpu.VMEM)
    v = pltpu.VMEM
    dma = pltpu.SemaphoreType.DMA
    outs = (((16, 384), F32), ((16, 384), F32), ((16, 2048), F32), ((3, 1, 384), F32), ((N, N, 2, 16, 384), BF16))
    results = pl.pallas_call(
        kernel,
        name="step",
        out_shape=tuple(pltpu.VMEM(*shape) for shape in outs),
        in_specs=[hbm] * 7,
        out_specs=(vmem,) * 5,
        scratch_shapes=[
            v((tokens, 384), BF16), v((tokens, 384), BF16), v((tokens, 512), BF16), v((2, tokens, 256), BF16),
            v((16, 384), F32), v((16, 2048), BF16), v((384, 384), BF16), v((16, 2048), F32), v((3, 1, 384), F32),
            v((N, 2, N, 16, 384), F32), v((N, N, 16, 384), F32),
            v((N, N, 16, 384), BF16), v((N, N - 1, 16, 384), BF16),
            v((N, 16, 384), BF16), v((N, N, 16, 384), BF16),
            v((4, 2, 2, N, 16, 384), BF16), v((2, N, N, 16, 384), BF16), v((2, N, N, 16, 384), BF16),
            v((2, N, N, 16, 384), F32), v((16, 384), F32), v((16, 384), F32),
            v((N, 1, 128), F32), v((4 * N, 1, 128), F32), v((2, 1, 128), F32),
            dma((7,)), pltpu.SemaphoreType.REGULAR((4,)),
            dma((3,)), dma((3,)), dma((N,)), dma((N,)), dma((N,)), dma((N,)), dma((N,)), dma((N,)),
            dma((N,)), dma((N,)), dma((N,)), dma((N,)), dma, dma,
            dma, dma((N,)), dma((N,)), dma((N,)), dma((N,)), dma((N,)), dma, dma((N,)),
            dma, dma, dma, dma((2, 4)), dma, dma, dma((3,)), dma((3,)),
        ],
        compiler_params=pltpu.CompilerParams(collective_id=0, has_side_effects=True),
    )(rnn_out, out_grad, weight, left_root[0], right_root[0], left_stat[0], jnp.transpose(right_stat, (1, 0, 2)))
    new_weight, step, left_new, right_new, copy = pl.pallas_call(
        write,
        name="write",
        out_shape=tuple(jax.ShapeDtypeStruct(*shape) for shape in outs),
        in_specs=[vmem] * 5,
        out_specs=(hbm,) * 5,
        scratch_shapes=[dma((N + 4,))],
    )(*(pltpu.with_memory_space_constraint(result, pltpu.VMEM) for result in results))
    return new_weight, step, left_new[None], jnp.transpose(right_new, (1, 0, 2)), copy.reshape(2048, 384)


def solution(mesh):
    torus = Mesh(mesh.devices.reshape(N, N, 2, mesh.shape["tp"]), ("fs_0", "fs_1", "fs_2", "tp"))
    return jax.shard_map(
        body,
        mesh=torus,
        in_specs=(
            P(FS, "tp"),
            P(FS, "tp"),
            P(FS, "tp"),
            P("tp", FS, None),
            P("tp", None, None),
            P("tp", FS, None),
            P("tp", FS, None),
        ),
        out_specs=(P(FS, "tp"), P(FS, "tp"), P("tp", FS, None), P("tp", FS, None), P(None, "tp")),
        check_vma=False,
    )
```
